32 devices in a mesh: sp: 8 (over z, x), tp: 4 (over y, core).
Axes of the slice: x: 2, y: 2, z: 4, core: 2. Of those that a mesh axis runs over, the one named last changes fastest.
Arguments:
- query_small: bfloat16 [6144, 1024], P('sp', 'tp'), may hold values from -6 to 6
- key_small: bfloat16 [6144, 1024], P('sp', 'tp'), may hold values from -6 to 6
- value_small: bfloat16 [6144, 1024], P('sp', 'tp'), may hold values from -6 to 6
- gates_small: float32 [6144, 16], P('sp', 'tp'), as said below
- query_large: bfloat16 [6144, 1024], P('sp', 'tp'), may hold values from -6 to 6
- key_large: bfloat16 [6144, 1024], P('sp', 'tp'), may hold values from -6 to 6
- value_large: bfloat16 [6144, 1024], P('sp', 'tp'), may hold values from -6 to 6
- gates_large: float32 [6144, 8], P('sp', 'tp'), as said below
- residual: bfloat16 [6144, 2048], P(('sp', 'tp')), may hold values from -6 to 6
- mixer_small: bfloat16 [1024, 2048], P('tp'), may hold values from -1 to 1
- mixer_large: bfloat16 [1024, 2048], P('tp'), may hold values from -1 to 1
- mix_gain: float32 [2048], replicated, may hold values from 0.1 to 1.9
- value_weight: bfloat16 [2048, 5632], P('sp', 'tp'), may hold values from -0.125 to 0.125
- gate_weight: bfloat16 [2048, 5632], P('sp', 'tp'), may hold values from -0.125 to 0.125
- value_taps: float32 [3, 5632], P(None, 'tp'), may hold values from -3 to 3
- gate_taps: float32 [3, 5632], P(None, 'tp'), may hold values from -3 to 3
- down_weight: bfloat16 [5632, 2048], P('tp', 'sp'), may hold values from -0.078125 to 0.078125
- final_gain: float32 [2048], replicated, may hold values from 0.1 to 1.9
Outputs:
- layer_out: bfloat16 [6144, 2048], P(('sp', 'tp'))
The draws below stay inside these ranges and needn't reach their ends.
Inputs may be any that keep to these rules, and one draw needn't show every extreme that they name: `gates_small`: each column never rises from one position to the next, and its first entry is negative. `gates_large`: each column never rises from one position to the next, and its first entry is negative.
All inputs are finite; a program needn't handle non-finite values.
Results may differ from the reference program's by a relative error of at most 0.018.
Values may be sent and summed in bfloat16 or wider, within the bound.
A program may use at most 128 MiB of HBM per device.

```python
import math
import jax
import jax.numpy as jnp
from jax import lax

D = 2048
FF = 5632
HS = 16
DS = 64
HL = 8
DL = 128
TOK_DEV = 768
SEQUENCE_TOKENS = 6144


def plant_pair(key, head_group, head_dim, salt):
    base_level = jax.random.fold_in(key, salt)
    width = head_group * head_dim
    queries = jnp.clip(jax.random.normal(jax.random.fold_in(base_level, 1), (SEQUENCE_TOKENS, width), jnp.float32), -6.0, 6.0)
    key_rows = jnp.clip(jax.random.normal(jax.random.fold_in(base_level, 2), (SEQUENCE_TOKENS, width), jnp.float32), -6.0, 6.0)
    return (queries, key_rows)


def gate_totals(key, head_group, salt):
    base_level = jax.random.fold_in(key, salt)
    share_fast = 0.5
    rapid_decay = jax.random.uniform(jax.random.fold_in(base_level, 1), (head_group,), jnp.float32) < share_fast
    rate = jnp.where(rapid_decay, 1.0 / 40.0, 0.5 / SEQUENCE_TOKENS)
    block_count = SEQUENCE_TOKENS // TOK_DEV
    factor = jnp.exp(jax.random.uniform(jax.random.fold_in(base_level, 2), (block_count, head_group), jnp.float32, -0.7, 0.7))
    factor = jnp.repeat(factor, TOK_DEV, axis=0)
    jitter = jax.random.uniform(jax.random.fold_in(base_level, 3), (SEQUENCE_TOKENS, head_group), jnp.float32, 0.3, 1.7)
    forget_decrements = rate[None, :] * factor * jitter
    spike_locations = jax.random.randint(jax.random.fold_in(base_level, 4), (3, head_group), 0, SEQUENCE_TOKENS)
    spike_magnitudes = jax.random.uniform(jax.random.fold_in(base_level, 5), (3, head_group), jnp.float32, 0.22, 0.69)
    token_positions = jnp.arange(SEQUENCE_TOKENS)
    match_events = jnp.where(token_positions[:, None, None] == spike_locations[None, :, :], spike_magnitudes[None, :, :], 0.0)
    spike_events = jnp.sum(match_events, axis=1) * jnp.where(rapid_decay, 0.0, 1.0)[None, :]
    return jnp.cumsum(-(forget_decrements + spike_events), axis=0)


def draw_query_small(key, part):
    return plant_pair(key, HS, DS, 11)[0].astype(jnp.bfloat16)


def draw_key_small(key, part):
    return plant_pair(key, HS, DS, 11)[1].astype(jnp.bfloat16)


def draw_query_large(key, part):
    return plant_pair(key, HL, DL, 23)[0].astype(jnp.bfloat16)


def draw_key_large(key, part):
    return plant_pair(key, HL, DL, 23)[1].astype(jnp.bfloat16)


def draw_gates_small(key, part):
    return gate_totals(key, HS, 37)


def draw_gates_large(key, part):
    return gate_totals(key, HL, 41)


def shard_levels(own_key, extent, pieces, low, largest):
    factor_of = 1.0
    for position, shards_of in pieces:
        heights = jax.random.uniform(jax.random.fold_in(jax.random.fold_in(own_key, 6), position), (shards_of,), jnp.float32, low / len(pieces), largest / len(pieces))
        factor_of = factor_of * jnp.repeat(jnp.exp(heights), extent[position] // shards_of).reshape((-1,) + (1,) * (len(extent) - 1 - position))
    return factor_of


def gaussian(stream_key, extent, scale, reach, split=(), kind=jnp.bfloat16):
    array = scale * jax.random.normal(stream_key, extent, jnp.float32)
    if split:
        array = array * shard_levels(stream_key, extent, split, -0.22, 0.18)
    return jnp.clip(array, -reach, reach).astype(kind)


def setup_inputs(seed: int = 0) -> dict:
    key_list = jax.random.split(jax.random.key(seed), 19)
    return {
        "query_small": draw_query_small(jax.random.fold_in(key_list[18], 71), 0),
        "key_small": draw_key_small(jax.random.fold_in(key_list[18], 71), 0),
        "value_small": gaussian(key_list[2], (SEQUENCE_TOKENS, HS * DS), 1.0, 6.0, ((0, 8), (1, 4))),
        "gates_small": draw_gates_small(jax.random.fold_in(key_list[18], 71), 0),
        "query_large": draw_query_large(jax.random.fold_in(key_list[18], 71), 0),
        "key_large": draw_key_large(jax.random.fold_in(key_list[18], 71), 0),
        "value_large": gaussian(key_list[6], (SEQUENCE_TOKENS, HL * DL), 1.0, 6.0, ((0, 8), (1, 4))),
        "gates_large": draw_gates_large(jax.random.fold_in(key_list[18], 71), 0),
        "residual": gaussian(key_list[8], (SEQUENCE_TOKENS, D), 1.0, 6.0, ((0, 32),)),
        "mixer_small": gaussian(key_list[9], (HS * DS, D), ((HS * DS + HL * DL) // 64) ** -0.5, 1.0, ((0, 4),)),
        "mixer_large": gaussian(key_list[10], (HL * DL, D), ((HS * DS + HL * DL) // 64) ** -0.5, 1.0, ((0, 4),)),
        "mix_gain": jnp.clip(1.0 + 0.18 * jax.random.normal(key_list[11], (D,), jnp.float32), 0.1, 1.9),
        "value_weight": gaussian(key_list[12], (D, FF), D ** -0.5, 0.125, ((0, 8), (1, 4))),
        "gate_weight": gaussian(key_list[13], (D, FF), D ** -0.5, 0.125, ((0, 8), (1, 4))),
        "value_taps": gaussian(key_list[14], (3, FF), 0.577, 3.0, ((1, 4),), jnp.float32),
        "gate_taps": gaussian(key_list[15], (3, FF), 0.577, 3.0, ((1, 4),), jnp.float32),
        "down_weight": gaussian(key_list[16], (FF, D), FF ** -0.5, 0.078125, ((0, 4), (1, 8))),
        "final_gain": jnp.clip(1.0 + 0.18 * jax.random.normal(key_list[17], (D,), jnp.float32), 0.1, 1.9),
    }


residual_scale = 2.0 ** 0.5
epsilon = 1e-05

def norm_rows(values, gain):
    center = lax.optimization_barrier(jnp.mean(values, axis=-1, keepdims=True))
    spread = lax.optimization_barrier(jnp.mean(jnp.square(values - center), axis=-1, keepdims=True))
    return (values - center) * lax.rsqrt(spread + epsilon) * gain.astype(jnp.float32)

def attend(queries, key_rows, value_rows, gates, head_dim):
    total_rows = queries.shape[0]
    heads_here = gates.shape[1]
    block_rows = math.gcd(total_rows, 256)
    block_count = total_rows // block_rows
    key_heads = key_rows.astype(jnp.float32).reshape(total_rows, heads_here, head_dim)
    value_heads = value_rows.astype(jnp.float32).reshape(total_rows, heads_here, head_dim)
    query_blocks = queries.reshape(block_count, block_rows, heads_here, head_dim)
    gate_blocks = gates.reshape(block_count, block_rows, heads_here)
    key_positions = jnp.arange(total_rows)

    def one_block(inputs):
        query_part, gate_part, first_row = inputs
        scores = jnp.einsum('qhd,khd->hqk', query_part.astype(jnp.float32), key_heads) * head_dim ** (-0.5)
        scores = scores + gate_part.T[:, :, None] - gates.T[:, None, :]
        token_positions = first_row + jnp.arange(block_rows)
        allowed = token_positions[:, None] >= key_positions[None, :]
        scores = jnp.where(allowed[None], scores, -jnp.inf)
        highest = lax.optimization_barrier(jnp.max(scores, axis=-1, keepdims=True))
        weights = jnp.exp(scores - highest)
        weight_sum = lax.optimization_barrier(jnp.sum(weights, axis=-1))
        rounded = lax.optimization_barrier(weights.astype(jnp.bfloat16)).astype(jnp.float32)
        output = jnp.einsum('hqk,khd->qhd', rounded, value_heads) / weight_sum.T[:, :, None]
        return output.astype(jnp.bfloat16)
    firsts = jnp.arange(block_count) * block_rows
    output = lax.map(one_block, (query_blocks, gate_blocks, firsts))
    return output.reshape(total_rows, heads_here * head_dim)

def causal_filter(rows_in, taps):
    values = rows_in.astype(jnp.float32)
    padded = jnp.concatenate([jnp.zeros((2, values.shape[1]), jnp.float32), values], axis=0)
    return taps[0] * padded[:-2] + taps[1] * padded[1:-1] + taps[2] * padded[2:]

def reference(query_small, key_small, value_small, gates_small, query_large, key_large, value_large, gates_large, residual, mixer_small, mixer_large, mix_gain, value_weight, gate_weight, value_taps, gate_taps, down_weight, final_gain):
    small_out = attend(query_small, key_small, value_small, gates_small, DS)
    large_out = attend(query_large, key_large, value_large, gates_large, DL)
    mix = jnp.dot(small_out, mixer_small, preferred_element_type=jnp.float32) + jnp.dot(large_out, mixer_large, preferred_element_type=jnp.float32)
    mixed = norm_rows(residual_scale * residual.astype(jnp.float32) + mix, mix_gain).astype(jnp.bfloat16)
    up_value = jnp.dot(mixed, value_weight, preferred_element_type=jnp.float32).astype(jnp.bfloat16)
    up_gate = jnp.dot(mixed, gate_weight, preferred_element_type=jnp.float32).astype(jnp.bfloat16)
    filt_value = causal_filter(up_value, value_taps)
    filt_gate = causal_filter(up_gate, gate_taps)
    hidden = (jax.nn.silu(filt_gate) * filt_value).astype(jnp.bfloat16)
    ffn = jnp.dot(hidden, down_weight, preferred_element_type=jnp.float32)
    return norm_rows(residual_scale * mixed.astype(jnp.float32) + ffn, final_gain).astype(jnp.bfloat16)
```

```python
import jax
import jax.numpy as jnp
from jax import lax
from jax.experimental import pallas as pl
from jax.experimental.pallas import tpu as pltpu
from jax.sharding import PartitionSpec as P


DS = 64
DL = 128


residual_scale = 2.0**0.5
epsilon = 1e-05


def passed_along(value, axis, steps):
    count = lax.axis_size(axis)
    first, last = (max(0, -steps), min(count, count - steps))
    return lax.ppermute(value, axis, [(source, source + steps) for source in range(first, last)])


def rotated(value, axis, steps):
    count = lax.axis_size(axis)
    return lax.ppermute(value, axis, [(s, (s + steps) % count) for s in range(count)])


def swapped(value, axis):
    return lax.ppermute(value, axis, [(s, s ^ 1) for s in range(lax.axis_size(axis))])


def norm_rows(values, gain):
    center = jnp.mean(values, axis=-1, keepdims=True)
    spread = jnp.mean(jnp.square(values - center), axis=-1, keepdims=True)
    return (values - center) * lax.rsqrt(spread + epsilon) * gain


def attend_body(small_count, diagonal, *refs):
    if diagonal:
        q_ref, k_ref, v_ref, gk_ref, gq_ref, peak_out, sum_out, acc_out = refs
    else:
        valid_ref, q_ref, k_ref, v_ref, gk_ref, gq_ref = refs[:6]
        peak_in, sum_in, acc_in, peak_out, sum_out, acc_out = refs[6:]
    head = pl.program_id(0)
    scale = jnp.where(head < small_count, DS ** (-0.5), DL ** (-0.5)).astype(jnp.float32)

    def logits():
        scores = lax.dot_general(
            q_ref[0], k_ref[...], (((1,), (1,)), ((), ())), preferred_element_type=jnp.float32
        )
        return scores * scale + (gq_ref[0] - gk_ref[0])

    if diagonal:
        scores = logits()
        query_rows = pl.program_id(1) * scores.shape[0]
        allowed = query_rows + lax.broadcasted_iota(
            jnp.int32, scores.shape, 0
        ) >= lax.broadcasted_iota(jnp.int32, scores.shape, 1)
        scores = jnp.where(allowed, scores, -jnp.inf)
        peak = jnp.max(scores, axis=-1, keepdims=True)
        weights = jnp.exp(scores - peak)
        peak_out[0] = peak
        sum_out[0] = jnp.sum(weights, axis=-1, keepdims=True)
        acc_out[0] = jnp.dot(
            weights.astype(jnp.bfloat16), v_ref[...], preferred_element_type=jnp.float32
        )
        return

    @pl.when(valid_ref[0] > 0)
    def _():
        scores = logits()
        peak = jnp.maximum(peak_in[0], jnp.max(scores, axis=-1, keepdims=True))
        factor = jnp.exp(peak_in[0] - peak)
        weights = jnp.exp(scores - peak)
        peak_out[0] = peak
        sum_out[0] = sum_in[0] * factor + jnp.sum(weights, axis=-1, keepdims=True)
        acc_out[0] = acc_in[0] * factor + jnp.dot(
            weights.astype(jnp.bfloat16), v_ref[...], preferred_element_type=jnp.float32
        )

    @pl.when(valid_ref[0] <= 0)
    def _():
        peak_out[0] = peak_in[0]
        sum_out[0] = sum_in[0]
        acc_out[0] = acc_in[0]


def attend(q_heads, key_value, key_gates, query_gates, small_count, state, valid):
    heads, rows, width = q_heads.shape
    per_small = width // DS
    groups = key_value.shape[1] // (2 * width)
    block = rows // 3 if rows % 3 == 0 and (rows // 3) % 128 == 0 else rows
    diagonal = state is None
    small_groups = small_count // per_small

    def group(h):
        return jnp.where(h < small_count, h // per_small, h - small_count + small_groups)

    per_query = pl.BlockSpec((1, block, 1), lambda h, i: (h, i, 0))
    wide = pl.BlockSpec((1, block, width), lambda h, i: (h, i, 0))
    in_specs = [
        wide,
        pl.BlockSpec((rows, width), lambda h, i: (0, group(h))),
        pl.BlockSpec((rows, width), lambda h, i: (0, groups + group(h))),
        pl.BlockSpec((1, 1, rows), lambda h, i: (h, 0, 0)),
        per_query,
    ]
    operands = [q_heads, key_value, key_value, key_gates[:, None, :], query_gates[:, :, None]]
    aliases = {}
    if not diagonal:
        in_specs = [pl.BlockSpec(memory_space=pltpu.SMEM)] + in_specs + [per_query, per_query, wide]
        operands = [valid] + operands + list(state)
        aliases = {6: 0, 7: 1, 8: 2}
    column = jax.ShapeDtypeStruct((heads, rows, 1), jnp.float32)

    def kernel(*refs):
        attend_body(small_count, diagonal, *refs)

    return pl.pallas_call(
        kernel,
        grid=(heads, rows // block),
        in_specs=in_specs,
        out_specs=[per_query, per_query, wide],
        out_shape=[column, column, jax.ShapeDtypeStruct((heads, rows, width), jnp.float32)],
        input_output_aliases=aliases,
        cost_estimate=pl.CostEstimate(
            flops=heads * rows * rows * width * 4,
            bytes_accessed=heads * rows * width * 12,
            transcendentals=heads * rows * rows,
        ),
        compiler_params=pltpu.CompilerParams(
            dimension_semantics=("arbitrary", "arbitrary"), vmem_limit_bytes=56 * 1024 * 1024
        ),
    )(*operands)


def per_device(
    query_small,
    key_small,
    value_small,
    gates_small,
    query_large,
    key_large,
    value_large,
    gates_large,
    residual,
    mixer_small,
    mixer_large,
    mix_gain,
    value_weight,
    gate_weight,
    value_taps,
    gate_taps,
    down_weight,
    final_gain,
):
    shard_rows = query_small.shape[0]
    sp_index = lax.axis_index("sp")
    tp_index = lax.axis_index("tp")
    tensor_parts = lax.axis_size("tp")
    sp_count = lax.axis_size("sp")
    splits = all(
        count % 2 == 0 and count * size % (2 * DL) == 0
        for count, size in ((gates_small.shape[1], DS), (gates_large.shape[1], DL))
    )
    team = 2 if splits and sp_count % 2 == 0 else 1
    pair_count = sp_count // team
    pair, side = sp_index // team, sp_index % team
    half_small = query_small.shape[1] // team
    small_count = gates_small.shape[1] // team
    large_count = gates_large.shape[1] // team

    def half(array, which):
        width = array.shape[1] // team
        return lax.dynamic_slice_in_dim(array, which * width, width, 1)

    def halves(parts, which):
        return jnp.concatenate([half(a, which) for a in parts], axis=1)

    def exchanged(parts):
        if team == 1:
            return jnp.concatenate(parts, axis=1)
        return in_order(halves(parts, side), swapped(halves(parts, 1 - side), "sp"), 0)

    def in_order(own, other, axis):
        return jnp.where(
            side == 0,
            jnp.concatenate([own, other], axis=axis),
            jnp.concatenate([other, own], axis=axis),
        )

    gate_parts = (gates_small, gates_large)
    key_value = exchanged((key_small, key_large, value_small, value_large))
    if team == 1:
        own_gates = jnp.concatenate(gate_parts, axis=1).T
    else:
        own_gates = in_order(
            halves(gate_parts, side).T, swapped(halves(gate_parts, 1 - side).T, "sp"), 1
        )
    queries = exchanged((query_small, query_large))

    width = DL
    per_small = width // DS
    lane_head = jnp.arange(width) // DS
    q_heads = []
    for h in range(small_count):
        columns = queries[:, (h // per_small) * width : (h // per_small + 1) * width]
        q_heads.append(jnp.where(lane_head == h % per_small, columns, 0).astype(jnp.bfloat16))
    for h in range(large_count):
        q_heads.append(queries[:, half_small + h * width : half_small + (h + 1) * width])
    q_heads = jnp.stack(q_heads)

    mixers = jnp.concatenate([mixer_small, mixer_large], axis=0)
    mixer_of = [mixers]
    for s in range(1, tensor_parts):
        mixer_of.append(rotated(mixers, "tp", -s))
    full_value = lax.all_gather(value_weight, "sp", axis=0, tiled=True)
    full_gate = lax.all_gather(gate_weight, "sp", axis=0, tiled=True)
    down_pieces = down_parts(down_weight)

    arriving, gates_arriving = [key_value], [own_gates]
    for step in range(1, pair_count):
        gates_arriving.append(passed_along(own_gates, "sp", step * team))
        arriving.append(passed_along(arriving[-1], "sp", team))
    state = attend(q_heads, key_value, own_gates, own_gates, small_count, None, None)
    for step in range(1, pair_count):
        valid = (pair >= step).astype(jnp.int32).reshape(1)
        state = attend(
            q_heads, arriving[step], gates_arriving[step], own_gates, small_count, state, valid
        )
    head_out = (state[2] / state[1]).astype(jnp.bfloat16)
    columns = []
    for g in range(small_count // per_small):
        merged = head_out[g * per_small]
        for h in range(1, per_small):
            merged = jnp.where(lane_head == h, head_out[g * per_small + h], merged)
        columns.append(merged)
    for h in range(large_count):
        columns.append(head_out[small_count + h])
    attended = jnp.concatenate(columns, axis=1)
    joined = attended
    if team == 2:
        own = lax.dynamic_slice_in_dim(attended, side * shard_rows, shard_rows, 0)
        other = swapped(
            lax.dynamic_slice_in_dim(attended, (1 - side) * shard_rows, shard_rows, 0), "sp"
        )
        joined = jnp.concatenate(
            [
                in_order(own[:, :half_small], other[:, :half_small], 1),
                in_order(own[:, half_small:], other[:, half_small:], 1),
            ],
            axis=1,
        )
    own_rows = shard_rows // tensor_parts
    arrived = lax.all_to_all(joined, "tp", split_axis=0, concat_axis=1, tiled=True)
    mix = jnp.zeros((own_rows, mixers.shape[1]), jnp.float32)
    for s in range(tensor_parts):
        source = (tp_index + s) % tensor_parts
        mix = mix + jnp.dot(
            lax.dynamic_slice_in_dim(arrived, source * joined.shape[1], joined.shape[1], 1),
            mixer_of[s],
            preferred_element_type=jnp.float32,
        )
    mixed = norm_rows(residual_scale * residual.astype(jnp.float32) + mix, mix_gain).astype(
        jnp.bfloat16
    )
    block_input = jnp.zeros((shard_rows, mixed.shape[1]), jnp.bfloat16)
    for s in range(tensor_parts):
        piece = mixed if s == 0 else rotated(mixed, "tp", -s)
        source = (tp_index + s) % tensor_parts
        block_input = lax.dynamic_update_slice_in_dim(block_input, piece, source * own_rows, 0)

    up_value = jnp.dot(block_input, full_value, preferred_element_type=jnp.float32).astype(
        jnp.bfloat16
    )
    up_gate = jnp.dot(block_input, full_gate, preferred_element_type=jnp.float32).astype(
        jnp.bfloat16
    )
    down_base, up_value = lax.optimization_barrier((down_weight, up_value))
    full_down = assembled(down_base, down_pieces)
    hidden_width = up_value.shape[1]
    trailing = jnp.concatenate([up_value[-2:], up_gate[-2:]], axis=1)
    earlier = passed_along(trailing, "sp", 1)
    padded_value = jnp.concatenate([earlier[:, :hidden_width], up_value], axis=0).astype(
        jnp.float32
    )
    padded_gate = jnp.concatenate([earlier[:, hidden_width:], up_gate], axis=0).astype(jnp.float32)
    filt_value = (
        value_taps[0] * padded_value[:-2]
        + value_taps[1] * padded_value[1:-1]
        + value_taps[2] * padded_value[2:]
    )
    filt_gate = (
        gate_taps[0] * padded_gate[:-2]
        + gate_taps[1] * padded_gate[1:-1]
        + gate_taps[2] * padded_gate[2:]
    )
    hidden = (jax.nn.silu(filt_gate) * filt_value).astype(jnp.bfloat16)

    def ffn_rows(s):
        target = (tp_index + s) % tensor_parts
        part = lax.dynamic_slice_in_dim(hidden, target * own_rows, own_rows, 0)
        return jnp.dot(part, full_down, preferred_element_type=jnp.float32)

    order = [tensor_parts // 2] + [s for s in range(1, tensor_parts) if s != tensor_parts // 2]
    received = [rotated(ffn_rows(s).astype(jnp.bfloat16), "tp", s) for s in order]
    ffn = ffn_rows(0)
    for part in received:
        ffn = ffn + part.astype(jnp.float32)
    return norm_rows(residual_scale * mixed.astype(jnp.float32) + ffn, final_gain).astype(
        jnp.bfloat16
    )


def down_parts(down_weight):
    pieces = []
    for s in range(1, lax.axis_size("sp")):
        pieces.append(rotated(down_weight, "sp", -s))
    return pieces


def assembled(own, pieces):
    count = lax.axis_size("sp")
    width = own.shape[1]
    index = lax.axis_index("sp")
    full = jnp.zeros((own.shape[0], count * width), own.dtype)
    for s, piece in enumerate([own] + pieces):
        full = lax.dynamic_update_slice_in_dim(full, piece, ((index + s) % count) * width, 1)
    return full


def solution(mesh):
    in_specs = (
        P("sp", "tp"),
        P("sp", "tp"),
        P("sp", "tp"),
        P("sp", "tp"),
        P("sp", "tp"),
        P("sp", "tp"),
        P("sp", "tp"),
        P("sp", "tp"),
        P(("sp", "tp"), None),
        P("tp", None),
        P("tp", None),
        P(),
        P("sp", "tp"),
        P("sp", "tp"),
        P(None, "tp"),
        P(None, "tp"),
        P("tp", "sp"),
        P(),
    )
    out_specs = P(("sp", "tp"), None)

    return jax.shard_map(
        per_device, mesh=mesh, in_specs=in_specs, out_specs=out_specs, check_vma=False
    )
```
